512 devices in a mesh: fs: 64 (over z, y), tp: 8 (over x, core).
Axes of the slice: x: 4, y: 8, z: 8, core: 2. Of those that a mesh axis runs over, the one named last changes fastest.
Arguments:
- saved_inputs: bfloat16 [49152, 2048], P('fs'), may hold values from -16 to 16
- cotangents: bfloat16 [3, 49152, 1024], P(None, 'fs', 'tp'), may hold values from -0.02734375 to 0.02734375
- left_roots: float32 [3, 2048, 2048], P(None, 'fs'), may hold values from -1 to 2
- right_roots: float32 [3, 1024, 128], P(None, 'tp'), may hold values from -1 to 2
- moments: float32 [3, 2048, 1024], P(None, 'fs', 'tp'), may hold values from -125 to 125
- masters: float32 [3, 2048, 1024], P(None, 'fs', 'tp'), may hold values from -3 to 3
Outputs:
- direction: float32 [3, 2048, 1024], P(None, 'fs', 'tp')
- moments_new: float32 [3, 2048, 1024], P(None, 'fs', 'tp')
- copies: bfloat16 [3, 2048, 1024], P(None, None, 'tp')
The draws below stay inside these ranges and needn't reach their ends.
All inputs are finite; a program needn't handle non-finite values.
Results may differ from the reference program's by a relative error of at most 0.002.
Values may be sent and summed in bfloat16 or wider, within the bound.
A program may use at most 64 MiB of HBM per device.

```python
import math
import jax
import jax.numpy as jnp
from jax import lax

D = 2048
SBW = 1024
RB = 128
TOKENS = 49152


def draw_left_roots(key, part):
    key_main = jax.random.fold_in(key, 11)
    raw_values = jax.random.normal(key_main, (3, D, D), jnp.float32)
    spread = 0.5 / math.sqrt(D)
    symmetric = (raw_values + jnp.transpose(raw_values, (0, 2, 1))) * (spread / math.sqrt(2.0))
    return (symmetric + jnp.eye(D, dtype=jnp.float32)[None]).astype(jnp.float32)


def draw_right_roots(key, part):
    key_main = jax.random.fold_in(key, 23)
    block_count = SBW // RB
    raw_values = jax.random.normal(key_main, (3, block_count, RB, RB), jnp.float32)
    spread = 0.5 / math.sqrt(RB)
    symmetric = (raw_values + jnp.transpose(raw_values, (0, 1, 3, 2))) * (spread / math.sqrt(2.0))
    blocks = symmetric + jnp.eye(RB, dtype=jnp.float32)[None, None]
    return blocks.reshape(3, SBW, RB).astype(jnp.float32)


def draw_moments(key, part):
    key_noise = jax.random.fold_in(key, 31)
    key_rows = jax.random.fold_in(key, 37)
    key_cols = jax.random.fold_in(key, 41)
    row_pos = jnp.arange(D, dtype=jnp.float32)[None, :, None] / D
    col_pos = jnp.arange(SBW, dtype=jnp.float32)[None, None, :] / SBW
    row_scale = 10.0 ** (0.5 * row_pos + 0.5 * jax.random.uniform(key_rows, (3, D, 1), jnp.float32))
    col_scale = 10.0 ** (0.5 * col_pos + 0.5 * jax.random.uniform(key_cols, (3, 1, SBW), jnp.float32))
    raw_values = jnp.clip(jax.random.normal(key_noise, (3, D, SBW), jnp.float32), -4.0, 4.0)
    return 0.3 * raw_values * row_scale * col_scale


def spiked(drawn, key, source, target, parts, factor):
    owner, partner = [(jnp.arange(drawn.shape[axis_at]) // (drawn.shape[axis_at] // parts)).reshape([-1 if axis == axis_at else 1 for axis in range(drawn.ndim)]) for axis_at in (source, target)]
    chosen = jax.random.permutation(key, parts)[partner]
    strong = (owner == chosen) | (owner == (partner + parts // 2) % parts)
    return jnp.where(strong, factor * drawn, drawn)


def level_of(stream_key, extent, shards, smallest, largest):
    gain, own = 1.0, jax.random.fold_in(stream_key, 6)
    for position, parts in shards:
        heights = jnp.exp(jax.random.uniform(jax.random.fold_in(own, position), (parts,), jnp.float32, smallest / len(shards), largest / len(shards)))
        gain = gain * jnp.repeat(heights, extent[position] // parts).reshape([-1 if axis == position else 1 for axis in range(len(extent))])
    return gain


def gaussian(rng, extent, scale, reach, cuts=(), kind=jnp.bfloat16):
    values = jax.random.normal(rng, extent, jnp.float32) * scale
    if len(cuts) > 0:
        values = level_of(rng, extent, cuts, -0.22, 0.18) * values
    return jnp.clip(values, min=-reach, max=reach).astype(kind)


def heavy_noise(key, extent, width, most, pieces, heavy, kind=jnp.bfloat16):
    array = width * jax.random.normal(key, extent, jnp.float32)
    if pieces:
        array = array * level_of(key, extent, pieces, -0.22, 0.18)
    return jnp.clip(spiked(array, jax.random.fold_in(key, 3), *heavy), -most, most).astype(kind)


def setup_inputs(seed: int = 0) -> dict:
    seeds = jax.random.split(jax.random.key(seed), 7)
    saved_inputs = heavy_noise(seeds[0], (TOKENS, D), 1.0, 16.0, ((0, 64),), (0, 1, 64, 4.0))
    cotangents = gaussian(seeds[1], (3, TOKENS, SBW), (TOKENS ** -0.5), 0.02734375, ((1, 64), (2, 8)))
    left_roots = draw_left_roots(jax.random.fold_in(seeds[6], 71), 0)
    right_roots = draw_right_roots(jax.random.fold_in(seeds[6], 71), 0)
    moments = draw_moments(jax.random.fold_in(seeds[6], 71), 0)
    masters = gaussian(seeds[5], (3, D, SBW), 0.5, 3.0, ((1, 64), (2, 8)), jnp.float32)
    return {"saved_inputs": saved_inputs, "cotangents": cotangents, "left_roots": left_roots, "right_roots": right_roots, "moments": moments, "masters": masters}


momentum_decay = 0.9
step_rate = 0.1
eps_value = 1e-06

def reference(saved_inputs, cotangents, left_roots, right_roots, moments, masters):
    gradients = jnp.einsum('td,mtc->mdc', saved_inputs.astype(jnp.float32), cotangents.astype(jnp.float32))
    left_done = jnp.einsum('mde,mec->mdc', left_roots, gradients, precision=lax.Precision.HIGHEST)
    block_count = SBW // RB
    right_blocks = right_roots.reshape(3, block_count, RB, RB)
    right_done = jnp.einsum('mdbi,mbij->mdbj', left_done.reshape(3, D, block_count, RB), right_blocks, precision=lax.Precision.HIGHEST).reshape(3, D, SBW)
    moments_new = momentum_decay * moments + right_done
    meansq = lax.optimization_barrier(jnp.mean(moments_new * moments_new, axis=(1, 2), keepdims=True))
    direction = moments_new * lax.rsqrt(meansq + eps_value)
    copies = (masters - step_rate * direction).astype(jnp.bfloat16)
    return (direction, moments_new, copies)
```

```python
import functools

import jax
import jax.numpy as jnp
from jax import lax
from jax.experimental import pallas as pl
from jax.experimental.pallas import tpu as pltpu
from jax.sharding import Mesh
from jax.sharding import PartitionSpec as P

Z, Y, X, CORE = "fs_0", "fs_1", "tp_0", "tp_1"
FS, TP = (Z, Y), (X, CORE)
MESH = pl.DeviceIdType.MESH
F32, BF16 = jnp.float32, jnp.bfloat16
M = 3
W = 128

momentum_decay = 0.9
step_rate = 0.1
eps_value = 1e-06


def far_first(n):
    return sorted(range(1, n), key=lambda o: -min(o, n - o))


def kernel(n, nx, nc, entries, x_hbm, c_hbm, l_hbm, rr_hbm, mo_hbm, ma_hbm,
           dir_hbm, mn_hbm, cp_hbm,
           xs, cv, ct, lv, ls, rr, mo, dirv, mnv, pb, own, rb, s2, g1, r2, gf,
           mal, mnl, sq1, sq2, sq3, cp,
           load_sem, out_sem, send_sem, rb_sem, r2_sem, ag_sem, gf_sem, ma_sem, mnl_sem,
           sq_sem1, sq_sem2, sq_sem3, cp_sem):
    z, y = lax.axis_index(Z), lax.axis_index(Y)
    x, core = lax.axis_index(X), lax.axis_index(CORE)
    nt = nx * nc
    t = x * nc + core
    c16 = W // n
    half = n // 2
    hr = mal.shape[3]
    big = ((Y, y), (Z, z))
    small = ((Z, z), (Y, y))
    sgn = 1 - 2 * core

    def at(i):
        return lax.rem(i + 2 * n, n)

    def remote(src, dst, ssem, rsem, where):
        return pltpu.make_async_remote_copy(
            src_ref=src, dst_ref=dst, send_sem=ssem, recv_sem=rsem,
            device_id=where, device_id_type=MESH)

    def got(dst, sem):
        pltpu.make_async_copy(dst, dst, sem).wait()

    barrier = pltpu.get_barrier_semaphore()

    order = []
    for k in range(half, 0, -1):
        order.append(("L", k))
        if k > 1:
            order.append(("S", k - 1))
    order.append(("O", 0))

    def block_of(h, kind, k):
        b = big[h][1]
        return at(b + sgn * k) if kind == "L" else at(b - sgn * k)

    def load(i, src, dst):
        copy = pltpu.make_async_copy(src, dst, load_sem.at[i])
        copy.start()
        return copy

    c_load = load(0, c_hbm, cv)
    x_loads = []
    for j, (kind, k) in enumerate(order):
        for h in range(2):
            col = pl.multiple_of(h * n * W + block_of(h, kind, k) * W, W)
            x_loads.append(load(1 + 2 * j + h, x_hbm.at[:, pl.ds(col, W)], xs.at[h, j]))
    base = 1 + 2 * n
    ma_loads = [load(base + h, ma_hbm.at[:, pl.ds(h * hr, hr), :],
                     mal.at[h, small[h][1]]) for h in range(2)]
    l_load = load(base + 2, l_hbm, lv)
    rr_load = load(base + 3, rr_hbm, rr)
    mo_load = load(base + 4, mo_hbm, mo)

    for name, me in ((Y, y), (Z, z)):
        for o in range(1, n):
            pl.semaphore_signal(barrier, inc=1, device_id={name: at(me + o)}, device_id_type=MESH)
    for o in range(1, nt):
        q = lax.rem(t + o, nt)
        pl.semaphore_signal(barrier, inc=1, device_id={X: q // nc, CORE: lax.rem(q, nc)},
                            device_id_type=MESH)

    c_load.wait()
    for m in range(M):
        ct[m * W:(m + 1) * W, :] = cv[m].T

    def ring_to(h, chain):
        name, b = big[h]
        return {name: at(b + sgn) if chain == "L" else at(b - sgn)}

    def slot(chain, s):
        return s - 1 if chain == "L" else half + s - 1

    def send_sum(h, chain, s, m):
        k = half + 1 - s if chain == "L" else half - s
        src = pb.at[h, block_of(h, chain, k), m]
        i = slot(chain, s)
        remote(src, rb.at[h, i, m], send_sem.at[0], rb_sem.at[h, i, m], ring_to(h, chain)).start()

    waited = False
    for j, (kind, k) in enumerate(order):
        for h in range(2):
            x_loads[2 * j + h].wait()
        both = jnp.concatenate([xs[0, j], xs[1, j]], axis=1)
        part = jnp.dot(ct[...], both, preferred_element_type=F32)
        for h in range(2):
            for m in range(M):
                piece = part[m * W:(m + 1) * W, h * W:(h + 1) * W]
                if kind == "O":
                    own[h, m] = piece
                else:
                    pb[h, block_of(h, kind, k), m] = piece.astype(BF16)
        if j == 0:
            pl.semaphore_wait(barrier, 2 * (n - 1) + nt - 1)
        if (kind, k) == ("L", half) or (kind, k) == ("S", half - 1):
            for m in range(M):
                for h in range(2):
                    send_sum(h, kind, 1, m)

    for h in range(2):
        ma_loads[h].wait()

    for s in range(2, half + 1):
        for m in range(M):
            for chain, last in (("L", half), ("S", half - 1)):
                if s > last:
                    continue
                k = half + 1 - s if chain == "L" else half - s
                for h in range(2):
                    i = slot(chain, s - 1)
                    got(rb.at[h, i, m], rb_sem.at[h, i, m])
                    b = block_of(h, chain, k)
                    pb[h, b, m] = (pb[h, b, m].astype(F32) + rb[h, i, m].astype(F32)).astype(BF16)
                    send_sum(h, chain, s, m)

    for m in range(M):
        for h in range(2):
            total = own[h, m]
            for chain, last in (("S", half - 1), ("L", half)):
                if last > 0:
                    i = slot(chain, last)
                    got(rb.at[h, i, m], rb_sem.at[h, i, m])
                    total = total + rb[h, i, m].astype(F32)
            g1[h, m] = total
            s2[h, m] = total.astype(BF16)

    peers = far_first(n)
    for o in peers:
        for h in range(2):
            name, me = small[h]
            q = at(me + o)
            rows = pl.ds(pl.multiple_of(q * c16, c16), c16)
            remote(s2.at[h, :, rows, :], r2.at[h, o - 1], send_sem.at[1], r2_sem.at[h, o - 1],
                   {name: q}).start()
    l_load.wait()
    rows_own = lv.shape[1]
    for m in range(M):
        value = lv[m]
        high = value.astype(BF16)
        ls[m, 0:rows_own, :] = high
        ls[m, rows_own:2 * rows_own, :] = (value - high.astype(F32)).astype(BF16)

    for h in range(2):
        name, me = small[h]
        rows = pl.ds(pl.multiple_of(me * c16, c16), c16)
        b = big[h][1]
        total = g1[h, :, rows, :]
        for o in range(1, n):
            got(r2.at[h, o - 1], r2_sem.at[h, o - 1])
            total = total + r2[h, o - 1].astype(F32)
        gf[h, b, :, rows, :] = total.astype(BF16)
        for o in peers:
            mine = gf.at[h, b, :, rows, :]
            remote(mine, mine, send_sem.at[2], ag_sem.at[h, o - 1], {name: at(me + o)}).start()

    for h in range(2):
        name, me = small[h]
        for o in peers:
            mine = mal.at[h, me]
            remote(mine, mine, send_sem.at[3], ma_sem.at[h, o - 1], {name: at(me + o)}).start()

    for h in range(2):
        name, me = small[h]
        for o in range(1, n):
            rows = pl.ds(pl.multiple_of(at(me - o) * c16, c16), c16)
            got(gf.at[h, big[h][1], :, rows, :], ag_sem.at[h, o - 1])

    def held(h, chain, s):
        b = big[h][1]
        return at(b - sgn * s) if chain == "L" else at(b + sgn * s)

    acc = [jnp.zeros((2 * rows_own, W), F32) for _ in range(M)]

    def add_block(h, b, m):
        cols = pl.ds(pl.multiple_of(h * n * W + b * W, W), W)
        acc[m] = acc[m] + lax.dot_general(
            ls[m, :, cols], gf[h, b, m], (((1,), (1,)), ((), ())), preferred_element_type=F32)

    def send_block(buffer, index, h, chain, s, m, number, sems):
        ref = index(buffer, h, held(h, chain, s - 1), m)
        remote(ref, ref, send_sem.at[number + h], sems.at[h, slot(chain, s), m], ring_to(h, chain)).start()

    def g_index(buffer, h, b, m):
        return buffer.at[h, b, m]

    def ring_gather(buffer, index, number, sems, arrived):
        for m in range(M):
            for h in range(2):
                for chain, last in (("L", half), ("S", half - 1)):
                    if last > 0:
                        send_block(buffer, index, h, chain, 1, m, number, sems)
        for m in range(M):
            for h in range(2):
                arrived(h, big[h][1], m)
        for s in range(1, half + 1):
            for m in range(M):
                came = []
                for chain, last in (("L", half), ("S", half - 1)):
                    if s > last:
                        continue
                    for h in range(2):
                        b = held(h, chain, s)
                        got(index(buffer, h, b, m), sems.at[h, slot(chain, s), m])
                        if s < last:
                            send_block(buffer, index, h, chain, s + 1, m, number, sems)
                        came.append((h, b))
                for h, b in came:
                    arrived(h, b, m)

    ring_gather(gf, g_index, 9, gf_sem, add_block)

    rr_load.wait()
    mo_load.wait()
    sums = []
    for m in range(M):
        left = acc[m][0:rows_own] + acc[m][rows_own:2 * rows_own]
        right = jnp.dot(left, rr[m], precision=lax.Precision.HIGHEST, preferred_element_type=F32)
        new = momentum_decay * mo[m] + right
        mnv[m] = new
        for h in range(2):
            mnl[h, small[h][1], m] = new[h * hr:(h + 1) * hr]
        sums.append(jnp.sum(new * new, axis=0, keepdims=True))
    sq1[y] = jnp.concatenate(sums + [jnp.zeros((8 - M, W), F32)], axis=0)

    for o in peers:
        remote(sq1.at[y], sq1.at[y], send_sem.at[5], sq_sem1.at[o - 1], {Y: at(y + o)}).start()
    out_copies = [pltpu.make_async_copy(mnv, mn_hbm, out_sem.at[0])]
    out_copies[0].start()
    for h in range(2):
        name, me = small[h]
        for o in peers:
            mine = mnl.at[h, me]
            remote(mine, mine, send_sem.at[6], mnl_sem.at[h, o - 1], {name: at(me + o)}).start()

    def summed(ref, count):
        total = ref[0]
        for i in range(1, count):
            total = total + ref[i]
        return total

    for o in range(1, n):
        got(sq1.at[at(y - o)], sq_sem1.at[o - 1])
    sq2[z] = summed(sq1, n)
    for o in peers:
        remote(sq2.at[z], sq2.at[z], send_sem.at[4], sq_sem2.at[o - 1], {Z: at(z + o)}).start()
    for o in range(1, n):
        got(sq2.at[at(z - o)], sq_sem2.at[o - 1])
    sq3[t] = summed(sq2, n)
    for o in range(1, nt):
        q = lax.rem(t + o, nt)
        remote(sq3.at[t], sq3.at[t], send_sem.at[7], sq_sem3.at[o - 1],
               {X: q // nc, CORE: lax.rem(q, nc)}).start()
    for h in range(2):
        name, me = small[h]
        for o in range(1, n):
            got(mal.at[h, at(me - o)], ma_sem.at[h, o - 1])
            got(mnl.at[h, at(me - o)], mnl_sem.at[h, o - 1])
    for o in range(1, nt):
        got(sq3.at[lax.rem(t - o + nt, nt)], sq_sem3.at[o - 1])
    totals = jnp.sum(summed(sq3, nt), axis=1, keepdims=True)
    scales = lax.rsqrt(totals / entries + eps_value)

    def c_index(buffer, h, b, m):
        return buffer.at[m, :, b, 0] if h == 0 else buffer.at[m, b, :, 1]

    for m in range(M):
        scale = scales[m:m + 1, :]
        for h in range(2):
            for i in range(n):
                value = (mal[h, i, m] - step_rate * (mnl[h, i, m] * scale)).astype(BF16)
                if h == 0:
                    cp[m, i, y, 0] = value
                else:
                    cp[m, z, i, 1] = value

    def put_out(h, b, m):
        pass

    ring_gather(cp, c_index, 11, cp_sem, put_out)
    for m in range(M):
        dirv[m] = mnv[m] * scales[m:m + 1, :]
    out_copies.append(pltpu.make_async_copy(dirv, dir_hbm, out_sem.at[1]))
    out_copies[1].start()
    out_copies.append(pltpu.make_async_copy(cp, cp_hbm, out_sem.at[2]))
    out_copies[2].start()

    got(rb, send_sem.at[0])
    got(r2, send_sem.at[1])
    got(r2, send_sem.at[2])
    for number, buffer in ((3, mal), (6, mnl)):
        got(buffer.at[:, 0:n - 1], send_sem.at[number])
    got(gf.at[0, 0:n - 1], send_sem.at[9])
    got(gf.at[1, 0:n - 1], send_sem.at[10])
    got(sq1.at[0:n - 1], send_sem.at[5])
    got(sq2.at[0:n - 1], send_sem.at[4])
    if nt > 1:
        got(sq3.at[0:nt - 1], send_sem.at[7])
    got(cp.at[:, 0:n - 1, :, 0], send_sem.at[11])
    got(cp.at[:, 0:n - 1, :, 1], send_sem.at[12])
    for copy in out_copies:
        copy.wait()


def update(n, nx, nc, x, c, l, rr, mo, ma):
    tokens, depth = x.shape
    rows_own = l.shape[1]
    hr = rows_own // 2
    c16 = W // n
    vmem, dma = pltpu.VMEM, pltpu.SemaphoreType.DMA
    nt = nx * nc
    peers = max(n - 1, 1)
    scratch = [
        vmem((2, n, tokens, W), BF16),
        vmem((M, tokens, W), BF16),
        vmem((M * W, tokens), BF16),
        vmem((M, rows_own, depth), F32),
        vmem((M, 2 * rows_own, depth), BF16),
        vmem((M, W, W), F32),
        vmem((M, rows_own, W), F32),
        vmem((M, rows_own, W), F32),
        vmem((M, rows_own, W), F32),
        vmem((2, n, M, W, W), BF16),
        vmem((2, M, W, W), F32),
        vmem((2, n - 1, M, W, W), BF16),
        vmem((2, M, W, W), BF16),
        vmem((2, M, W, W), F32),
        vmem((2, n - 1, M, c16, W), BF16),
        vmem((2, n, M, W, W), BF16),
        vmem((2, n, M, hr, W), F32),
        vmem((2, n, M, hr, W), F32),
        vmem((n, 8, W), F32),
        vmem((n, 8, W), F32),
        vmem((nt, 8, W), F32),
        vmem((M, n, n, 2, hr, W), BF16),
        dma((1 + 2 * n + 5,)),
        dma((3,)),
        dma((13,)),
        dma((2, n - 1, M)),
        dma((2, n - 1)),
        dma((2, n - 1)),
        dma((2, n - 1, M)),
        dma((2, n - 1)),
        dma((2, n - 1)),
        dma((peers,)), dma((peers,)), dma((max(nt - 1, 1),)),
        dma((2, n - 1, M)),
    ]
    small = jax.ShapeDtypeStruct((M, rows_own, W), F32)
    any_ = pl.BlockSpec(memory_space=pl.ANY)
    direction, new, copies = pl.pallas_call(
        functools.partial(kernel, n, nx, nc, float(depth * W * nt)),
        out_shape=(small, small, jax.ShapeDtypeStruct((M, n, n, 2, hr, W), BF16)),
        in_specs=[any_] * 6,
        out_specs=(any_,) * 3,
        scratch_shapes=scratch,
        name="update",
        compiler_params=pltpu.CompilerParams(
            collective_id=0, has_side_effects=True, vmem_limit_bytes=60 * 1024 * 1024),
    )(x, c, l, rr, mo, ma)
    return direction, new, copies.reshape(M, n * n * rows_own, W)


def solution(mesh):
    n, nx, nc = 8, 4, 2
    torus = Mesh(mesh.devices.reshape(n, n, nx, nc), (Z, Y, X, CORE))
    in_specs = (
        P(FS, None),
        P(None, FS, TP),
        P(None, FS, None),
        P(None, TP, None),
        P(None, FS, TP),
        P(None, FS, TP),
    )
    out_specs = (P(None, FS, TP), P(None, FS, TP), P(None, None, TP))
    return jax.shard_map(
        functools.partial(update, n, nx, nc),
        mesh=torus, in_specs=in_specs, out_specs=out_specs, check_vma=False)
```

```python
import functools

import jax
import jax.numpy as jnp
from jax import lax
from jax.experimental import pallas as pl
from jax.experimental.pallas import tpu as pltpu
from jax.sharding import Mesh
from jax.sharding import PartitionSpec as P

Z, Y, X, CORE = "fs_0", "fs_1", "tp_0", "tp_1"
FS, TP = (Z, Y), (X, CORE)
MESH = pl.DeviceIdType.MESH
F32, BF16 = jnp.float32, jnp.bfloat16
M = 3
W = 128
PARTS = 2

momentum_decay = 0.9
step_rate = 0.1
eps_value = 1e-06


def far_first(n):
    return sorted(range(1, n), key=lambda o: -min(o, n - o))


def kernel(n, nx, nc, entries, x_hbm, c_hbm, l_hbm, rr_hbm, mo_hbm, ma_hbm,
           dirv, mnv, cp,
           xs, cv, ct, lv, ls, rr, mo, pb, own, rb, s2, g1, r2, gf, lt, lp, lr,
           mal, mnl, sq1, sq2, sq3,
           load_sem, send_sem, rb_sem, r2_sem, ag_sem, lt_sem, lx_sem, lr_sem, ma_sem, mnl_sem,
           sq_sem1, sq_sem2, sq_sem3, cp_sem):
    z, y = lax.axis_index(Z), lax.axis_index(Y)
    x, core = lax.axis_index(X), lax.axis_index(CORE)
    nt = nx * nc
    t = x * nc + core
    c16 = W // n
    half = n // 2
    rows_own = lv.shape[1]
    peers = far_first(n)
    hr = mal.shape[3]
    big = ((Y, y), (Z, z))
    small = ((Z, z), (Y, y))
    sgn = 1 - 2 * core

    def at(i):
        return lax.rem(i + 2 * n, n)

    def remote(src, dst, ssem, rsem, where):
        return pltpu.make_async_remote_copy(
            src_ref=src, dst_ref=dst, send_sem=ssem, recv_sem=rsem,
            device_id=where, device_id_type=MESH)

    def got(dst, sem):
        pltpu.make_async_copy(dst, dst, sem).wait()

    barrier = pltpu.get_barrier_semaphore()

    order = []
    for k in range(half, 0, -1):
        order.append(("L", k))
        if k > 1:
            order.append(("S", k - 1))
    order.append(("O", 0))

    def block_of(h, kind, k):
        b = big[h][1]
        return at(b + sgn * k) if kind == "L" else at(b - sgn * k)

    def load(i, src, dst):
        copy = pltpu.make_async_copy(src, dst, load_sem.at[i])
        copy.start()
        return copy

    c_load = load(0, c_hbm, cv)
    x_loads = []
    for j, (kind, k) in enumerate(order):
        for h in range(2):
            col = pl.multiple_of(h * n * W + block_of(h, kind, k) * W, W)
            x_loads.append(load(1 + 2 * j + h, x_hbm.at[:, pl.ds(col, W)], xs.at[h, j]))
    base = 1 + 2 * n
    ma_loads = [load(base + h, ma_hbm.at[:, pl.ds(h * hr, hr), :],
                     mal.at[h, small[h][1]]) for h in range(2)]
    l_load = load(base + 2, l_hbm, lv)
    rr_load = load(base + 3, rr_hbm, rr)
    mo_load = load(base + 4, mo_hbm, mo)

    for name, me in ((Y, y), (Z, z)):
        for o in range(1, n):
            pl.semaphore_signal(barrier, inc=1, device_id={name: at(me + o)}, device_id_type=MESH)
    for o in range(1, nt):
        q = lax.rem(t + o, nt)
        pl.semaphore_signal(barrier, inc=1, device_id={X: q // nc, CORE: lax.rem(q, nc)},
                            device_id_type=MESH)

    c_load.wait()
    for m in range(M):
        ct[m * W:(m + 1) * W, :] = cv[m].T

    def ring_to(h, chain):
        name, b = big[h]
        return {name: at(b + sgn) if chain == "L" else at(b - sgn)}

    def slot(chain, s):
        return s - 1 if chain == "L" else half + s - 1

    cp_rows = W // PARTS

    def send_sum(h, chain, s, m, p):
        k = half + 1 - s if chain == "L" else half - s
        rows = pl.ds(p * cp_rows, cp_rows)
        src = pb.at[h, block_of(h, chain, k), m, rows]
        i = slot(chain, s)
        remote(src, rb.at[h, i, m, rows], send_sem.at[0], rb_sem.at[h, i, m * PARTS + p],
               ring_to(h, chain)).start()

    def got_sum(h, i, m, p):
        rows = pl.ds(p * cp_rows, cp_rows)
        got(rb.at[h, i, m, rows], rb_sem.at[h, i, m * PARTS + p])
        return rb[h, i, m, rows].astype(F32)

    waited = False
    for j, (kind, k) in enumerate(order):
        for h in range(2):
            x_loads[2 * j + h].wait()
        both = jnp.concatenate([xs[0, j], xs[1, j]], axis=1)
        part = jnp.dot(ct[...], both, preferred_element_type=F32)
        for h in range(2):
            for m in range(M):
                piece = part[m * W:(m + 1) * W, h * W:(h + 1) * W]
                if kind == "O":
                    own[h, m] = piece
                else:
                    pb[h, block_of(h, kind, k), m] = piece.astype(BF16)
        if j == 0:
            pl.semaphore_wait(barrier, 2 * (n - 1) + nt - 1)
        if (kind, k) == ("L", half) or (kind, k) == ("S", half - 1):
            for m in range(M):
                for p in range(PARTS):
                    for h in range(2):
                        send_sum(h, kind, 1, m, p)

    share = rows_own // nx
    part_rows = pl.ds(pl.multiple_of(x * share, share), share)
    l_load.wait()
    for o in peers:
        for h in range(2):
            name, me = big[h]
            q = at(me + o)
            cols = pl.ds(pl.multiple_of(h * n * W + q * W, W), W)
            remote(lv.at[:, part_rows, cols], lt.at[h, o - 1, :, part_rows, :], send_sem.at[8],
                   lt_sem.at[h, o - 1], {name: q}).start()

    for s in range(2, half + 1):
        for m in range(M):
            for p in range(PARTS):
                rows = pl.ds(p * cp_rows, cp_rows)
                for chain, last in (("L", half), ("S", half - 1)):
                    if s > last:
                        continue
                    k = half + 1 - s if chain == "L" else half - s
                    for h in range(2):
                        came = got_sum(h, slot(chain, s - 1), m, p)
                        b = block_of(h, chain, k)
                        pb[h, b, m, rows] = (pb[h, b, m, rows].astype(F32) + came).astype(BF16)
                        send_sum(h, chain, s, m, p)

    for m in range(M):
        for p in range(PARTS):
            rows = pl.ds(p * cp_rows, cp_rows)
            for h in range(2):
                total = own[h, m, rows]
                for chain, last in (("S", half - 1), ("L", half)):
                    if last > 0:
                        total = total + got_sum(h, slot(chain, last), m, p)
                g1[h, m, rows] = total
                s2[h, m, rows] = total.astype(BF16)

    for o in peers:
        for h in range(2):
            name, me = small[h]
            q = at(me + o)
            rows = pl.ds(pl.multiple_of(q * c16, c16), c16)
            remote(s2.at[h, :, rows, :], r2.at[h, o - 1], send_sem.at[1], r2_sem.at[h, o - 1],
                   {name: q}).start()
    for h in range(2):
        for o in range(1, n):
            got(lt.at[h, o - 1, :, part_rows, :], lt_sem.at[h, o - 1])
    for o in range(1, nx):
        mine = lt.at[:, :, :, part_rows, :]
        remote(mine, mine, send_sem.at[9], lx_sem.at[o - 1], {X: lax.rem(x + o, nx)}).start()
    for h in range(2):
        name, me = small[h]
        ma_loads[h].wait()
        for o in peers:
            mine = mal.at[h, me]
            remote(mine, mine, send_sem.at[3], ma_sem.at[h, o - 1], {name: at(me + o)}).start()

    def split_left(h, m, o, value):
        high = value.astype(BF16)
        ls[h, m, 2 * o * rows_own:(2 * o + 1) * rows_own, :] = high
        low = (value - high.astype(F32)).astype(BF16)
        ls[h, m, (2 * o + 1) * rows_own:(2 * o + 2) * rows_own, :] = low

    for h in range(2):
        cols = pl.ds(pl.multiple_of(h * n * W + big[h][1] * W, W), W)
        for m in range(M):
            split_left(h, m, 0, lv[m, :, cols])

    for h in range(2):
        name, me = small[h]
        rows = pl.ds(pl.multiple_of(me * c16, c16), c16)
        total = g1[h, :, rows, :]
        for o in range(1, n):
            got(r2.at[h, o - 1], r2_sem.at[h, o - 1])
            total = total + r2[h, o - 1].astype(F32)
        gf[h, :, rows, :] = total.astype(BF16)
        for o in peers:
            mine = gf.at[h, :, rows, :]
            remote(mine, mine, send_sem.at[2], ag_sem.at[h, o - 1], {name: at(me + o)}).start()

    for o in range(1, nx):
        theirs = pl.ds(pl.multiple_of(lax.rem(x + nx - o, nx) * share, share), share)
        got(lt.at[:, :, :, theirs, :], lx_sem.at[o - 1])
    for h in range(2):
        for o in range(1, n):
            for m in range(M):
                split_left(h, m, o, lt[h, o - 1, m])

    left = [jnp.zeros((rows_own, W), F32) for _ in range(M)]
    for h in range(2):
        name, me = small[h]
        for o in range(1, n):
            rows = pl.ds(pl.multiple_of(at(me - o) * c16, c16), c16)
            got(gf.at[h, :, rows, :], ag_sem.at[h, o - 1])
        for m in range(M):
            both = lax.dot_general(ls[h, m], gf[h, m], (((1,), (1,)), ((), ())),
                                   preferred_element_type=F32)
            for o in range(n):
                high = both[2 * o * rows_own:(2 * o + 1) * rows_own]
                value = high + both[(2 * o + 1) * rows_own:(2 * o + 2) * rows_own]
                if o == 0:
                    left[m] = left[m] + value
                else:
                    lp[h, o - 1, m] = value.astype(BF16)
        name, me = big[h]
        for o in peers:
            remote(lp.at[h, o - 1], lr.at[h, o - 1], send_sem.at[10], lr_sem.at[h, o - 1],
                   {name: at(me - o)}).start()
    for h in range(2):
        for o in range(1, n):
            got(lr.at[h, o - 1], lr_sem.at[h, o - 1])
            for m in range(M):
                left[m] = left[m] + lr[h, o - 1, m].astype(F32)

    rr_load.wait()
    mo_load.wait()
    sums = []
    for m in range(M):
        right = jnp.dot(left[m], rr[m], precision=lax.Precision.HIGHEST, preferred_element_type=F32)
        new = momentum_decay * mo[m] + right
        mnv[m] = new
        for h in range(2):
            mnl[h, small[h][1], m] = new[h * hr:(h + 1) * hr]
        sums.append(jnp.sum(new * new, axis=0, keepdims=True))
    sq1[y] = jnp.concatenate(sums + [jnp.zeros((8 - M, W), F32)], axis=0)

    for o in peers:
        remote(sq1.at[y], sq1.at[y], send_sem.at[5], sq_sem1.at[o - 1], {Y: at(y + o)}).start()
    for h in range(2):
        name, me = small[h]
        for o in peers:
            mine = mnl.at[h, me]
            remote(mine, mine, send_sem.at[6], mnl_sem.at[h, o - 1], {name: at(me + o)}).start()

    def summed(ref, count):
        total = ref[0]
        for i in range(1, count):
            total = total + ref[i]
        return total

    for o in range(1, n):
        got(sq1.at[at(y - o)], sq_sem1.at[o - 1])
    sq2[z] = summed(sq1, n)
    for o in peers:
        remote(sq2.at[z], sq2.at[z], send_sem.at[4], sq_sem2.at[o - 1], {Z: at(z + o)}).start()
    for o in range(1, n):
        got(sq2.at[at(z - o)], sq_sem2.at[o - 1])
    sq3[t] = summed(sq2, n)
    for o in range(1, nt):
        q = lax.rem(t + o, nt)
        remote(sq3.at[t], sq3.at[t], send_sem.at[7], sq_sem3.at[o - 1],
               {X: q // nc, CORE: lax.rem(q, nc)}).start()
    for h in range(2):
        name, me = small[h]
        for o in range(1, n):
            got(mal.at[h, at(me - o)], ma_sem.at[h, o - 1])
            got(mnl.at[h, at(me - o)], mnl_sem.at[h, o - 1])
    for o in range(1, nt):
        got(sq3.at[lax.rem(t - o + nt, nt)], sq_sem3.at[o - 1])
    totals = jnp.sum(summed(sq3, nt), axis=1, keepdims=True)
    scales = lax.rsqrt(totals / entries + eps_value)

    def make_copies(h, m, p):
        for i in range(p * lines, (p + 1) * lines):
            scale = scales[m:m + 1, :]
            value = (mal[h, i, m] - step_rate * (mnl[h, i, m] * scale)).astype(BF16)
            if h == 0:
                cp[m, i, y, 0] = value
            else:
                cp[m, z, i, 1] = value

    def held(h, chain, s):
        b = big[h][1]
        return at(b - sgn * s) if chain == "L" else at(b + sgn * s)

    lines = n // PARTS if n >= PARTS else n

    def c_piece(h, b, m, p):
        part = pl.ds(p * lines, lines)
        return cp.at[m, part, b, 0] if h == 0 else cp.at[m, b, part, 1]

    def send_copy(h, chain, s, m, p):
        ref = c_piece(h, held(h, chain, s - 1), m, p)
        remote(ref, ref, send_sem.at[11 + h], cp_sem.at[h, slot(chain, s), m * PARTS + p],
               ring_to(h, chain)).start()

    for m in range(M):
        for p in range(PARTS):
            for h in range(2):
                make_copies(h, m, p)
            for h in range(2):
                send_copy(h, "L", 1, m, p)
                if half > 1:
                    send_copy(h, "S", 1, m, p)
    for m in range(M):
        dirv[m] = mnv[m] * scales[m:m + 1, :]
    for s in range(1, half + 1):
        for m in range(M):
            for p in range(PARTS):
                for chain, last in (("L", half), ("S", half - 1)):
                    if s > last:
                        continue
                    for h in range(2):
                        got(c_piece(h, held(h, chain, s), m, p),
                            cp_sem.at[h, slot(chain, s), m * PARTS + p])
                        if s < last:
                            send_copy(h, chain, s + 1, m, p)

    got(rb, send_sem.at[0])
    got(r2, send_sem.at[1])
    got(r2, send_sem.at[2])
    for number, buffer in ((3, mal), (6, mnl)):
        got(buffer.at[:, 0:n - 1], send_sem.at[number])
    got(lt.at[:, :, :, part_rows, :], send_sem.at[8])
    for o in range(1, nx):
        got(lt.at[:, :, :, pl.ds((o - 1) * share, share), :], send_sem.at[9])
    got(lr, send_sem.at[10])
    got(sq1.at[0:n - 1], send_sem.at[5])
    got(sq2.at[0:n - 1], send_sem.at[4])
    if nt > 1:
        got(sq3.at[0:nt - 1], send_sem.at[7])
    got(cp.at[:, 0:n - 1, :, 0], send_sem.at[11])
    got(cp.at[:, 0:n - 1, :, 1], send_sem.at[12])


def write_out(*refs):
    ins, outs, sem = refs[:3], refs[3:6], refs[6]
    copies = [pltpu.make_async_copy(a, b, sem.at[i]) for i, (a, b) in enumerate(zip(ins, outs))]
    for copy in copies[::-1]:
        copy.start()
    for copy in copies:
        copy.wait()


def update(n, nx, nc, x, c, l, rr, mo, ma):
    tokens, depth = x.shape
    rows_own = l.shape[1]
    hr = rows_own // 2
    c16 = W // n
    vmem, dma = pltpu.VMEM, pltpu.SemaphoreType.DMA
    nt = nx * nc
    peers = max(n - 1, 1)
    scratch = [
        vmem((2, n, tokens, W), BF16),
        vmem((M, tokens, W), BF16),
        vmem((M * W, tokens), BF16),
        vmem((M, rows_own, depth), F32),
        vmem((2, M, 2 * n * rows_own, W), BF16),
        vmem((M, W, W), F32),
        vmem((M, rows_own, W), F32),
        vmem((2, n, M, W, W), BF16),
        vmem((2, M, W, W), F32),
        vmem((2, n - 1, M, W, W), BF16),
        vmem((2, M, W, W), BF16),
        vmem((2, M, W, W), F32),
        vmem((2, n - 1, M, c16, W), BF16),
        vmem((2, M, W, W), BF16),
        vmem((2, n - 1, M, rows_own, W), F32),
        vmem((2, n - 1, M, rows_own, W), BF16),
        vmem((2, n - 1, M, rows_own, W), BF16),
        vmem((2, n, M, hr, W), F32),
        vmem((2, n, M, hr, W), F32),
        vmem((n, 8, W), F32),
        vmem((n, 8, W), F32),
        vmem((nt, 8, W), F32),
        dma((1 + 2 * n + 5,)),
        dma((13,)),
        dma((2, n - 1, M * PARTS)),
        dma((2, n - 1)),
        dma((2, n - 1)),
        dma((2, n - 1)),
        dma((max(nx - 1, 1),)),
        dma((2, n - 1)),
        dma((2, n - 1)),
        dma((2, n - 1)),
        dma((peers,)), dma((peers,)), dma((max(nt - 1, 1),)),
        dma((2, n - 1, M * PARTS)),
    ]
    small = jax.ShapeDtypeStruct((M, rows_own, W), F32)
    any_ = pl.BlockSpec(memory_space=pl.ANY)
    hbm = pl.BlockSpec(memory_space=pltpu.HBM)
    local = pl.BlockSpec(memory_space=pltpu.VMEM)
    shapes = (small, small, jax.ShapeDtypeStruct((M, n, n, 2, hr, W), BF16))
    x, c, l, rr, mo, ma = [pltpu.with_memory_space_constraint(v, pltpu.HBM) for v in (x, c, l, rr, mo, ma)]
    held = pl.pallas_call(
        functools.partial(kernel, n, nx, nc, float(depth * W * nt)),
        out_shape=shapes,
        in_specs=[hbm] * 6,
        out_specs=(local,) * 3,
        scratch_shapes=scratch,
        name="update",
        compiler_params=pltpu.CompilerParams(
            collective_id=0, has_side_effects=True, vmem_limit_bytes=40960 * 1024),
    )(x, c, l, rr, mo, ma)
    direction, new, copies = pl.pallas_call(
        write_out,
        out_shape=shapes,
        in_specs=[local] * 3,
        out_specs=(any_,) * 3,
        scratch_shapes=[dma((3,))],
        name="write_out",
        compiler_params=pltpu.CompilerParams(vmem_limit_bytes=8 * 1024 * 1024),
    )(*held)
    return direction, new, copies.reshape(M, n * n * rows_own, W)


def solution(mesh):
    n, nx, nc = 8, 4, 2
    torus = Mesh(mesh.devices.reshape(n, n, nx, nc), (Z, Y, X, CORE))
    in_specs = (
        P(FS, None),
        P(None, FS, TP),
        P(None, FS, None),
        P(None, TP, None),
        P(None, FS, TP),
        P(None, FS, TP),
    )
    out_specs = (P(None, FS, TP), P(None, FS, TP), P(None, None, TP))
    return jax.shard_map(
        functools.partial(update, n, nx, nc),
        mesh=torus, in_specs=in_specs, out_specs=out_specs, check_vma=False)
```

```python
import functools

import jax
import jax.numpy as jnp
from jax import lax
from jax.experimental import pallas as pl
from jax.experimental.pallas import tpu as pltpu
from jax.sharding import Mesh
from jax.sharding import PartitionSpec as P

Z, Y, X, CORE = "fs_0", "fs_1", "tp_0", "tp_1"
FS, TP = (Z, Y), (X, CORE)
MESH = pl.DeviceIdType.MESH
F32, BF16 = jnp.float32, jnp.bfloat16
M = 3
W = 128
PARTS = 2

momentum_decay = 0.9
step_rate = 0.1
eps_value = 1e-06


def far_first(n):
    return sorted(range(1, n), key=lambda o: -min(o, n - o))


def kernel(n, nx, nc, entries, x_hbm, c_hbm, l_hbm, rr_hbm, mo_hbm, ma_hbm,
           dirv, mnv, cp,
           xs, cv, ct, lv, ls, rr, mo, pb, own, rb, s2, g1, r2, gf, lt, lp, lr,
           mal, mnl, sq1, sq2, sq3,
           load_sem, send_sem, rb_sem, r2_sem, ag_sem, lt_sem, lx_sem, lr_sem, ma_sem, mnl_sem,
           sq_sem1, sq_sem2, sq_sem3, cp_sem):
    z, y = lax.axis_index(Z), lax.axis_index(Y)
    x, core = lax.axis_index(X), lax.axis_index(CORE)
    nt = nx * nc
    t = x * nc + core
    c16 = W // n
    half = n // 2
    rows_own = lv.shape[1]
    peers = far_first(n)
    hr = mal.shape[3]
    big = ((Y, y), (Z, z))
    small = ((Z, z), (Y, y))
    sgn = 1 - 2 * core

    def at(i):
        return lax.rem(i + 2 * n, n)

    def remote(src, dst, ssem, rsem, where):
        return pltpu.make_async_remote_copy(
            src_ref=src, dst_ref=dst, send_sem=ssem, recv_sem=rsem,
            device_id=where, device_id_type=MESH)

    def got(dst, sem):
        pltpu.make_async_copy(dst, dst, sem).wait()

    barrier = pltpu.get_barrier_semaphore()

    skip = half >= 2

    def terms(chain, k):
        top = half if chain == "L" else half - 1
        if chain == "L" and skip:
            if k >= half - 1:
                return []
            if k == half - 2:
                return [half - 1, half]
        return [k + 1] if k < top else []

    def hop(chain, k):
        return 2 if chain == "L" and skip and k == half else 1

    order = [("L", half)]
    for k in range(half - 1, 0, -1):
        order += [("L", k), ("S", k)]
    order.append(("O", 0))

    def block_of(h, kind, k):
        b = big[h][1]
        return at(b + sgn * k) if kind == "L" else at(b - sgn * k)

    def load(i, src, dst):
        copy = pltpu.make_async_copy(src, dst, load_sem.at[i])
        copy.start()
        return copy

    c_load = load(0, c_hbm, cv)
    x_loads = []
    for j, (kind, k) in enumerate(order):
        for h in range(2):
            col = pl.multiple_of(h * n * W + block_of(h, kind, k) * W, W)
            x_loads.append(load(1 + 2 * j + h, x_hbm.at[:, pl.ds(col, W)], xs.at[h, j]))
    base = 1 + 2 * n
    ma_loads = [load(base + h, ma_hbm.at[:, pl.ds(h * hr, hr), :],
                     mal.at[h, small[h][1]]) for h in range(2)]
    l_load = load(base + 2, l_hbm, lv)
    rr_load = load(base + 3, rr_hbm, rr)
    mo_load = load(base + 4, mo_hbm, mo)

    for name, me in ((Y, y), (Z, z)):
        for o in range(1, n):
            pl.semaphore_signal(barrier, inc=1, device_id={name: at(me + o)}, device_id_type=MESH)
    for o in range(1, nt):
        q = lax.rem(t + o, nt)
        pl.semaphore_signal(barrier, inc=1, device_id={X: q // nc, CORE: lax.rem(q, nc)},
                            device_id_type=MESH)

    c_load.wait()
    for m in range(M):
        ct[m * W:(m + 1) * W, :] = cv[m].T

    def ring_to(h, chain, links=1):
        name, b = big[h]
        return {name: at(b + links * sgn) if chain == "L" else at(b - links * sgn)}

    def slot(chain, s):
        return s - 1 if chain == "L" else half + s - 1

    cp_rows = W // PARTS

    def send_sum(h, chain, k, m, p):
        rows = pl.ds(p * cp_rows, cp_rows)
        src = pb.at[h, block_of(h, chain, k), m, rows]
        i = slot(chain, k)
        remote(src, rb.at[h, i, m, rows], send_sem.at[0], rb_sem.at[h, i, m * PARTS + p],
               ring_to(h, chain, hop(chain, k))).start()

    def got_sum(h, i, m, p):
        rows = pl.ds(p * cp_rows, cp_rows)
        got(rb.at[h, i, m, rows], rb_sem.at[h, i, m * PARTS + p])
        return rb[h, i, m, rows].astype(F32)

    waited = False
    for j, (kind, k) in enumerate(order):
        for h in range(2):
            x_loads[2 * j + h].wait()
        both = jnp.concatenate([xs[0, j], xs[1, j]], axis=1)
        part = jnp.dot(ct[...], both, preferred_element_type=F32)
        for h in range(2):
            for m in range(M):
                piece = part[m * W:(m + 1) * W, h * W:(h + 1) * W]
                if kind == "O":
                    own[h, m] = piece
                else:
                    pb[h, block_of(h, kind, k), m] = piece.astype(BF16)
        if j == 0:
            pl.semaphore_wait(barrier, 2 * (n - 1) + nt - 1)
        if kind != "O" and not terms(kind, k):
            for m in range(M):
                for p in range(PARTS):
                    for h in range(2):
                        send_sum(h, kind, k, m, p)

    share = rows_own // nx
    part_rows = pl.ds(pl.multiple_of(x * share, share), share)
    l_load.wait()
    for o in peers:
        for h in range(2):
            name, me = big[h]
            q = at(me + o)
            cols = pl.ds(pl.multiple_of(h * n * W + q * W, W), W)
            remote(lv.at[:, part_rows, cols], lt.at[h, o - 1, :, part_rows, :], send_sem.at[8],
                   lt_sem.at[h, o - 1], {name: q}).start()

    for k in range(half - 1, 0, -1):
        for m in range(M):
            for p in range(PARTS):
                rows = pl.ds(p * cp_rows, cp_rows)
                for chain in ("L", "S"):
                    if not terms(chain, k):
                        continue
                    for h in range(2):
                        b = block_of(h, chain, k)
                        total = pb[h, b, m, rows].astype(F32)
                        for far in terms(chain, k):
                            total = total + got_sum(h, slot(chain, far), m, p)
                        pb[h, b, m, rows] = total.astype(BF16)
                        send_sum(h, chain, k, m, p)

    for m in range(M):
        for p in range(PARTS):
            rows = pl.ds(p * cp_rows, cp_rows)
            for h in range(2):
                total = own[h, m, rows]
                for chain in ("S", "L"):
                    for far in terms(chain, 0):
                        total = total + got_sum(h, slot(chain, far), m, p)
                g1[h, m, rows] = total
                s2[h, m, rows] = total.astype(BF16)

    for o in peers:
        for h in range(2):
            name, me = small[h]
            q = at(me + o)
            rows = pl.ds(pl.multiple_of(q * c16, c16), c16)
            remote(s2.at[h, :, rows, :], r2.at[h, o - 1], send_sem.at[1], r2_sem.at[h, o - 1],
                   {name: q}).start()
    for h in range(2):
        for o in range(1, n):
            got(lt.at[h, o - 1, :, part_rows, :], lt_sem.at[h, o - 1])
    for o in range(1, nx):
        mine = lt.at[:, :, :, part_rows, :]
        remote(mine, mine, send_sem.at[9], lx_sem.at[o - 1], {X: lax.rem(x + o, nx)}).start()

    def split_left(h, m, o, value):
        high = value.astype(BF16)
        ls[h, m, 2 * o * rows_own:(2 * o + 1) * rows_own, :] = high
        low = (value - high.astype(F32)).astype(BF16)
        ls[h, m, (2 * o + 1) * rows_own:(2 * o + 2) * rows_own, :] = low

    for h in range(2):
        cols = pl.ds(pl.multiple_of(h * n * W + big[h][1] * W, W), W)
        for m in range(M):
            split_left(h, m, 0, lv[m, :, cols])

    for h in range(2):
        name, me = small[h]
        rows = pl.ds(pl.multiple_of(me * c16, c16), c16)
        total = g1[h, :, rows, :]
        for o in range(1, n):
            got(r2.at[h, o - 1], r2_sem.at[h, o - 1])
            total = total + r2[h, o - 1].astype(F32)
        gf[h, :, rows, :] = total.astype(BF16)
        for o in peers:
            mine = gf.at[h, :, rows, :]
            remote(mine, mine, send_sem.at[2], ag_sem.at[h, o - 1], {name: at(me + o)}).start()

    for o in range(1, nx):
        theirs = pl.ds(pl.multiple_of(lax.rem(x + nx - o, nx) * share, share), share)
        got(lt.at[:, :, :, theirs, :], lx_sem.at[o - 1])
    for h in range(2):
        for o in range(1, n):
            for m in range(M):
                split_left(h, m, o, lt[h, o - 1, m])

    left = [jnp.zeros((rows_own, W), F32) for _ in range(M)]
    for h in range(2):
        name, me = small[h]
        for o in range(1, n):
            rows = pl.ds(pl.multiple_of(at(me - o) * c16, c16), c16)
            got(gf.at[h, :, rows, :], ag_sem.at[h, o - 1])
        for m in range(M):
            both = lax.dot_general(ls[h, m], gf[h, m], (((1,), (1,)), ((), ())),
                                   preferred_element_type=F32)
            for o in range(n):
                high = both[2 * o * rows_own:(2 * o + 1) * rows_own]
                value = high + both[(2 * o + 1) * rows_own:(2 * o + 2) * rows_own]
                if o == 0:
                    left[m] = left[m] + value
                else:
                    lp[h, o - 1, m] = value.astype(BF16)
        name, me = big[h]
        for o in peers:
            remote(lp.at[h, o - 1], lr.at[h, o - 1], send_sem.at[10], lr_sem.at[h, o - 1],
                   {name: at(me - o)}).start()
    for h in range(2):
        for o in range(1, n):
            got(lr.at[h, o - 1], lr_sem.at[h, o - 1])
            for m in range(M):
                left[m] = left[m] + lr[h, o - 1, m].astype(F32)

    rr_load.wait()
    mo_load.wait()
    sums = []
    for m in range(M):
        right = jnp.dot(left[m], rr[m], precision=lax.Precision.HIGHEST, preferred_element_type=F32)
        new = momentum_decay * mo[m] + right
        mnv[m] = new
        for h in range(2):
            mnl[h, small[h][1], m] = new[h * hr:(h + 1) * hr]
        sums.append(jnp.sum(new * new, axis=0, keepdims=True))
    sq1[y] = jnp.concatenate(sums + [jnp.zeros((8 - M, W), F32)], axis=0)

    for o in peers:
        remote(sq1.at[y], sq1.at[y], send_sem.at[5], sq_sem1.at[o - 1], {Y: at(y + o)}).start()
    for h in range(2):
        name, me = small[h]
        for o in peers:
            mine = mnl.at[h, me]
            remote(mine, mine, send_sem.at[6], mnl_sem.at[h, o - 1], {name: at(me + o)}).start()

    def summed(ref, count):
        total = ref[0]
        for i in range(1, count):
            total = total + ref[i]
        return total

    for o in range(1, n):
        got(sq1.at[at(y - o)], sq_sem1.at[o - 1])
    sq2[z] = summed(sq1, n)
    for o in peers:
        remote(sq2.at[z], sq2.at[z], send_sem.at[4], sq_sem2.at[o - 1], {Z: at(z + o)}).start()
    for h in range(2):
        name, me = small[h]
        ma_loads[h].wait()
        for o in peers:
            mine = mal.at[h, me]
            remote(mine, mine, send_sem.at[3], ma_sem.at[h, o - 1], {name: at(me + o)}).start()
    for o in range(1, n):
        got(sq2.at[at(z - o)], sq_sem2.at[o - 1])
    sq3[t] = summed(sq2, n)
    for o in range(1, nt):
        q = lax.rem(t + o, nt)
        remote(sq3.at[t], sq3.at[t], send_sem.at[7], sq_sem3.at[o - 1],
               {X: q // nc, CORE: lax.rem(q, nc)}).start()
    for h in range(2):
        name, me = small[h]
        for o in range(1, n):
            got(mal.at[h, at(me - o)], ma_sem.at[h, o - 1])
            got(mnl.at[h, at(me - o)], mnl_sem.at[h, o - 1])
    for o in range(1, nt):
        got(sq3.at[lax.rem(t - o + nt, nt)], sq_sem3.at[o - 1])
    totals = jnp.sum(summed(sq3, nt), axis=1, keepdims=True)
    scales = lax.rsqrt(totals / entries + eps_value)

    def make_copies(h, m, p):
        for i in range(p * lines, (p + 1) * lines):
            scale = scales[m:m + 1, :]
            value = (mal[h, i, m] - step_rate * (mnl[h, i, m] * scale)).astype(BF16)
            if h == 0:
                cp[m, i, y, 0] = value
            else:
                cp[m, z, i, 1] = value

    def held(h, chain, s):
        b = big[h][1]
        return at(b - sgn * s) if chain == "L" else at(b + sgn * s)

    lines = n // PARTS if n >= PARTS else n

    def c_piece(h, b, m, p):
        part = pl.ds(p * lines, lines)
        return cp.at[m, part, b, 0] if h == 0 else cp.at[m, b, part, 1]

    def send_copy(h, chain, s, m, p):
        links = hop(chain, s)
        ref = c_piece(h, held(h, chain, s - links), m, p)
        remote(ref, ref, send_sem.at[11 + h], cp_sem.at[h, slot(chain, s), m * PARTS + p],
               ring_to(h, chain, links)).start()

    def pass_on(h, chain, s, m, p):
        last = half if chain == "L" else half - 1
        for to in range(s + 1, last + 1):
            if to - hop(chain, to) == s:
                send_copy(h, chain, to, m, p)

    for m in range(M):
        for p in range(PARTS):
            for h in range(2):
                make_copies(h, m, p)
            for h in range(2):
                pass_on(h, "L", 0, m, p)
                pass_on(h, "S", 0, m, p)
    for m in range(M):
        dirv[m] = mnv[m] * scales[m:m + 1, :]
    for s in range(1, half + 1):
        for m in range(M):
            for p in range(PARTS):
                for chain, last in (("L", half), ("S", half - 1)):
                    if s > last:
                        continue
                    for h in range(2):
                        got(c_piece(h, held(h, chain, s), m, p),
                            cp_sem.at[h, slot(chain, s), m * PARTS + p])
                        pass_on(h, chain, s, m, p)

    got(rb, send_sem.at[0])
    got(r2, send_sem.at[1])
    got(r2, send_sem.at[2])
    for number, buffer in ((3, mal), (6, mnl)):
        got(buffer.at[:, 0:n - 1], send_sem.at[number])
    got(lt.at[:, :, :, part_rows, :], send_sem.at[8])
    for o in range(1, nx):
        got(lt.at[:, :, :, pl.ds((o - 1) * share, share), :], send_sem.at[9])
    got(lr, send_sem.at[10])
    got(sq1.at[0:n - 1], send_sem.at[5])
    got(sq2.at[0:n - 1], send_sem.at[4])
    if nt > 1:
        got(sq3.at[0:nt - 1], send_sem.at[7])
    got(cp.at[:, 0:n - 1, :, 0], send_sem.at[11])
    got(cp.at[:, 0:n - 1, :, 1], send_sem.at[12])


def write_out(*refs):
    ins, outs, sem = refs[:3], refs[3:6], refs[6]
    copies = [pltpu.make_async_copy(a, b, sem.at[i]) for i, (a, b) in enumerate(zip(ins, outs))]
    for copy in copies[::-1]:
        copy.start()
    for copy in copies:
        copy.wait()


def update(n, nx, nc, x, c, l, rr, mo, ma):
    tokens, depth = x.shape
    rows_own = l.shape[1]
    hr = rows_own // 2
    c16 = W // n
    vmem, dma = pltpu.VMEM, pltpu.SemaphoreType.DMA
    nt = nx * nc
    peers = max(n - 1, 1)
    scratch = [
        vmem((2, n, tokens, W), BF16),
        vmem((M, tokens, W), BF16),
        vmem((M * W, tokens), BF16),
        vmem((M, rows_own, depth), F32),
        vmem((2, M, 2 * n * rows_own, W), BF16),
        vmem((M, W, W), F32),
        vmem((M, rows_own, W), F32),
        vmem((2, n, M, W, W), BF16),
        vmem((2, M, W, W), F32),
        vmem((2, n - 1, M, W, W), BF16),
        vmem((2, M, W, W), BF16),
        vmem((2, M, W, W), F32),
        vmem((2, n - 1, M, c16, W), BF16),
        vmem((2, M, W, W), BF16),
        vmem((2, n - 1, M, rows_own, W), F32),
        vmem((2, n - 1, M, rows_own, W), BF16),
        vmem((2, n - 1, M, rows_own, W), BF16),
        vmem((2, n, M, hr, W), F32),
        vmem((2, n, M, hr, W), F32),
        vmem((n, 8, W), F32),
        vmem((n, 8, W), F32),
        vmem((nt, 8, W), F32),
        dma((1 + 2 * n + 5,)),
        dma((13,)),
        dma((2, n - 1, M * PARTS)),
        dma((2, n - 1)),
        dma((2, n - 1)),
        dma((2, n - 1)),
        dma((max(nx - 1, 1),)),
        dma((2, n - 1)),
        dma((2, n - 1)),
        dma((2, n - 1)),
        dma((peers,)), dma((peers,)), dma((max(nt - 1, 1),)),
        dma((2, n - 1, M * PARTS)),
    ]
    small = jax.ShapeDtypeStruct((M, rows_own, W), F32)
    any_ = pl.BlockSpec(memory_space=pl.ANY)
    hbm = pl.BlockSpec(memory_space=pltpu.HBM)
    local = pl.BlockSpec(memory_space=pltpu.VMEM)
    shapes = (small, small, jax.ShapeDtypeStruct((M, n, n, 2, hr, W), BF16))
    x, c, l, rr, mo, ma = [pltpu.with_memory_space_constraint(v, pltpu.HBM) for v in (x, c, l, rr, mo, ma)]
    held = pl.pallas_call(
        functools.partial(kernel, n, nx, nc, float(depth * W * nt)),
        out_shape=shapes,
        in_specs=[hbm] * 6,
        out_specs=(local,) * 3,
        scratch_shapes=scratch,
        name="update",
        compiler_params=pltpu.CompilerParams(
            collective_id=0, has_side_effects=True, vmem_limit_bytes=40960 * 1024),
    )(x, c, l, rr, mo, ma)
    direction, new, copies = pl.pallas_call(
        write_out,
        out_shape=shapes,
        in_specs=[local] * 3,
        out_specs=(any_,) * 3,
        scratch_shapes=[dma((3,))],
        name="write_out",
        compiler_params=pltpu.CompilerParams(vmem_limit_bytes=8 * 1024 * 1024),
    )(*held)
    return direction, new, copies.reshape(M, n * n * rows_own, W)


def solution(mesh):
    n, nx, nc = 8, 4, 2
    torus = Mesh(mesh.devices.reshape(n, n, nx, nc), (Z, Y, X, CORE))
    in_specs = (
        P(FS, None),
        P(None, FS, TP),
        P(None, FS, None),
        P(None, TP, None),
        P(None, FS, TP),
        P(None, FS, TP),
    )
    out_specs = (P(None, FS, TP), P(None, FS, TP), P(None, None, TP))
    return jax.shard_map(
        functools.partial(update, n, nx, nc),
        mesh=torus, in_specs=in_specs, out_specs=out_specs, check_vma=False)
```
